512 devices in a mesh: sp: 128 (over z, y, core), tp: 4 (over x).
Axes of the slice: x: 4, y: 8, z: 8, core: 2. Of those that a mesh axis runs over, the one named last changes fastest.
Arguments:
- tokens: bfloat16 [65536, 2048], P('sp'), may hold values from -6 to 6
- norm_gain: bfloat16 [2048], replicated, may hold values from 0.099609375 to 1.8984375
- w_conv_value: bfloat16 [2048, 2048], P('sp', 'tp'), may hold values from -0.125 to 0.125
- w_conv_gate: bfloat16 [2048, 2048], P('sp', 'tp'), may hold values from -0.125 to 0.125
- w_query: bfloat16 [2048, 2048], P('sp', 'tp'), may hold values from -0.125 to 0.125
- w_key: bfloat16 [2048, 512], P('sp', 'tp'), may hold values from -0.125 to 0.125
- w_value: bfloat16 [2048, 512], P('sp', 'tp'), may hold values from -0.125 to 0.125
- conv_taps: float32 [31, 2048], P(None, 'tp'), as said below
- ln_gain: float32 [2048], P('tp'), may hold values from 0.1 to 1.9
- sinks: float32 [32], P('tp'), may hold values from 3 to 6
- out_conv: bfloat16 [2048, 2048], P('tp', 'sp'), may hold values from -0.125 to 0.125
- out_attn: bfloat16 [2048, 2048], P('tp', 'sp'), may hold values from -0.5 to 0.5
Outputs:
- mixed: bfloat16 [65536, 2048], P(('sp', 'tp'))
- log_sums: float32 [32, 65536], P('tp', 'sp')
The draws below stay inside these ranges and needn't reach their ends.
Inputs may be any that keep to these rules, and one draw needn't show every extreme that they name: `conv_taps`: each tap lies within 30 / sqrt(31) in magnitude.
All inputs are finite; a program needn't handle non-finite values.
Results may differ from the reference program's by a relative error of at most 0.017.
Values may be sent and summed in bfloat16 or wider, within the bound.
A program may use at most 64 MiB of HBM per device.

```python
import jax
import jax.numpy as jnp
from jax import lax

D = 2048
CONV_CH = 2048
HEADS = 32
KV_HEADS = 8
HEAD_DIM = 64
CONV_K = 31
WINDOW = 128
TOKENS = 65536
SPLITS = 4


def draw_conv_taps(key, part):
    channel = jnp.arange(CONV_CH, dtype=jnp.float32)
    samples = jax.random.truncated_normal(key, -3.0, 3.0, (CONV_K, CONV_CH), jnp.float32)
    scales = 10.0 ** (channel / CONV_CH)
    return samples * scales[None, :] * CONV_K ** (-0.5)


def steps_of(own_key, extent, split, low, top_value):
    def one(position, shards_of):
        steps = jax.random.uniform(jax.random.fold_in(jax.random.fold_in(own_key, 6), position), (shards_of,), jnp.float32, low / len(split), top_value / len(split))
        return jnp.repeat(jnp.exp(steps), extent[position] // shards_of).reshape((-1,) + (1,) * (len(extent) - position - 1))

    gain = one(*split[0])
    for cut in split[1:]:
        gain = gain * one(*cut)
    return gain


def noise(rng, shape, spread, most, pieces=(), held_as=jnp.bfloat16):
    array = spread * jax.random.normal(rng, shape, jnp.float32)
    if pieces:
        array = array * steps_of(rng, shape, pieces, -0.22, 0.18)
    return jnp.clip(array, -most, most).astype(held_as)


def setup_inputs(seed: int = 0) -> dict:
    arg_keys = jax.random.split(jax.random.key(seed), 13)
    tokens = noise(arg_keys[0], (TOKENS, D), 1.0, 6.0, ((0, 128),))
    norm_gain = jnp.clip(1.0 + 0.18 * jax.random.normal(arg_keys[1], (D,), jnp.float32), 0.099609375, 1.8984375).astype(jnp.bfloat16)
    w_conv_value = noise(arg_keys[2], (D, CONV_CH), D ** -0.5, 0.125, ((0, 128), (1, 4)))
    w_conv_gate = noise(arg_keys[3], (D, CONV_CH), D ** -0.5, 0.125, ((0, 128), (1, 4)))
    w_query = noise(arg_keys[4], (D, HEADS * HEAD_DIM), D ** -0.5, 0.125, ((0, 128), (1, 4)))
    w_key = noise(arg_keys[5], (D, KV_HEADS * HEAD_DIM), D ** -0.5, 0.125, ((0, 128), (1, 4)))
    w_value = noise(arg_keys[6], (D, KV_HEADS * HEAD_DIM), D ** -0.5, 0.125, ((0, 128), (1, 4)))
    conv_taps = draw_conv_taps(jax.random.fold_in(arg_keys[12], 71), 0)
    ln_gain = jnp.clip(1.0 + 0.18 * jax.random.normal(arg_keys[8], (CONV_CH,), jnp.float32), 0.1, 1.9)
    sinks = jnp.clip(3.0 + 3.0 * jax.random.uniform(arg_keys[9], (HEADS,), jnp.float32) ** steps_of(arg_keys[9], (HEADS,), ((0, 4),), -0.2, 0.2), 3.0, 6.0)
    out_conv = noise(arg_keys[10], (CONV_CH, D), CONV_CH ** -0.5, 0.125, ((0, 4), (1, 128)))
    out_attn = noise(arg_keys[11], (HEADS * HEAD_DIM, D), (HEADS * HEAD_DIM // 16) ** -0.5, 0.5, ((0, 4), (1, 128)))
    return dict(tokens=tokens, norm_gain=norm_gain, w_conv_value=w_conv_value, w_conv_gate=w_conv_gate, w_query=w_query, w_key=w_key, w_value=w_value, conv_taps=conv_taps, ln_gain=ln_gain, sinks=sinks, out_conv=out_conv, out_attn=out_attn)


NORM_EPS = 1e-06
CHANNEL_EPS = 1e-05
ROPE_BASE = 10000.0

def rotate(heads, positions):
    half_dim = heads.shape[-1] // 2
    inverse = ROPE_BASE ** (-jnp.arange(half_dim, dtype=jnp.float32) / half_dim)
    angles = positions.astype(jnp.float32)[:, None] * inverse[None, :]
    cosine = jnp.cos(angles)[:, None, :]
    sine = jnp.sin(angles)[:, None, :]
    as_float = heads.astype(jnp.float32)
    front_part = as_float[..., :half_dim]
    back_part = as_float[..., half_dim:]
    return jnp.concatenate([front_part * cosine - back_part * sine, back_part * cosine + front_part * sine], axis=-1)

def reference(tokens, norm_gain, w_conv_value, w_conv_gate, w_query, w_key, w_value, conv_taps, ln_gain, sinks, out_conv, out_attn):
    as_float = tokens.astype(jnp.float32)
    normed = (as_float * lax.rsqrt(lax.optimization_barrier(jnp.mean(as_float * as_float, axis=-1, keepdims=True)) + NORM_EPS) * norm_gain.astype(jnp.float32)).astype(jnp.bfloat16)

    def project(weight):
        return jnp.dot(normed, weight, preferred_element_type=jnp.float32).astype(jnp.bfloat16)
    conv_value = project(w_conv_value)
    conv_gate = project(w_conv_gate)
    query_raw = project(w_query)
    key_raw = project(w_key)
    value_rows = project(w_value)
    glu = (conv_value.astype(jnp.float32) * jax.nn.sigmoid(conv_gate.astype(jnp.float32))).astype(jnp.bfloat16)
    padded = jnp.concatenate([jnp.zeros((CONV_K - 1, CONV_CH), jnp.float32), glu.astype(jnp.float32)], axis=0)
    conv_out = jnp.zeros((TOKENS, CONV_CH), jnp.float32)
    for tap in range(CONV_K):
        conv_out = conv_out + conv_taps[tap].astype(jnp.float32)[None, :] * padded[tap:tap + TOKENS]
    mean = lax.optimization_barrier(jnp.mean(conv_out, axis=-1, keepdims=True))
    var = lax.optimization_barrier(jnp.mean(conv_out * conv_out, axis=-1, keepdims=True)) - mean * mean
    conv_branch = jax.nn.silu((conv_out - mean) * lax.rsqrt(var + CHANNEL_EPS) * ln_gain.astype(jnp.float32)[None, :]).astype(jnp.bfloat16)
    positions = jnp.arange(TOKENS, dtype=jnp.int32)
    query = rotate(query_raw.reshape(TOKENS, HEADS, HEAD_DIM), positions).astype(jnp.bfloat16)
    key = rotate(key_raw.reshape(TOKENS, KV_HEADS, HEAD_DIM), positions).astype(jnp.bfloat16)
    values = value_rows.reshape(TOKENS, KV_HEADS, HEAD_DIM)
    group = HEADS // KV_HEADS
    blocks = TOKENS // WINDOW
    q_blocks = query.reshape(blocks, WINDOW, KV_HEADS, group, HEAD_DIM).astype(jnp.float32)
    leading = jnp.zeros((WINDOW, KV_HEADS, HEAD_DIM), jnp.bfloat16)
    key_blocks = jnp.concatenate([leading, key], axis=0).reshape(blocks + 1, WINDOW, KV_HEADS, HEAD_DIM)
    value_blocks = jnp.concatenate([leading, values], axis=0).reshape(blocks + 1, WINDOW, KV_HEADS, HEAD_DIM)
    key_window = jnp.concatenate([key_blocks[:-1], key_blocks[1:]], axis=1).astype(jnp.float32)
    value_window = jnp.concatenate([value_blocks[:-1], value_blocks[1:]], axis=1).astype(jnp.float32)
    scores = jnp.einsum('nqhgd,nkhd->nhgqk', q_blocks, key_window) * HEAD_DIM ** (-0.5)
    query_index = jnp.arange(WINDOW)[:, None] + WINDOW
    key_index = jnp.arange(2 * WINDOW)[None, :]
    band = (key_index <= query_index) & (query_index - key_index < WINDOW)
    block_index = jnp.arange(blocks)[:, None, None]
    allowed = band[None] & (block_index * WINDOW + key_index[None] - WINDOW >= 0)
    allowed = allowed[:, None, None]
    totals = lax.optimization_barrier(jnp.sum(jnp.where(allowed, jnp.exp(scores), 0.0), axis=-1))
    totals = totals + jnp.exp(sinks.astype(jnp.float32)).reshape(1, KV_HEADS, group, 1)
    log_total = jnp.log(totals)
    weights = jnp.where(allowed, jnp.exp(scores - log_total[..., None]), 0.0).astype(jnp.bfloat16)
    attended = jnp.einsum('nhgqk,nkhd->nqhgd', weights.astype(jnp.float32), value_window)
    attn_branch = attended.astype(jnp.bfloat16).reshape(TOKENS, HEADS * HEAD_DIM)
    log_sums = log_total.transpose(1, 2, 0, 3).reshape(HEADS, TOKENS)
    conv_width = CONV_CH // SPLITS
    attn_width = HEADS * HEAD_DIM // SPLITS
    mixed = jnp.zeros((TOKENS, D), jnp.float32)
    for index in range(SPLITS):
        part_sum = jnp.dot(conv_branch[:, index * conv_width:(index + 1) * conv_width], out_conv[index * conv_width:(index + 1) * conv_width], preferred_element_type=jnp.float32)
        part_sum = part_sum + jnp.dot(attn_branch[:, index * attn_width:(index + 1) * attn_width], out_attn[index * attn_width:(index + 1) * attn_width], preferred_element_type=jnp.float32)
        rounded = lax.optimization_barrier(part_sum.astype(jnp.bfloat16))
        mixed = mixed + rounded.astype(jnp.float32)
    return (mixed.astype(jnp.bfloat16), log_sums)
```

```python
import jax
import jax.numpy as jnp
from jax import lax
from jax.experimental import pallas as pl
from jax.experimental.pallas import tpu as pltpu
from jax.sharding import PartitionSpec as P

CONV_CH = 2048
HEADS = 32
KV_HEADS = 8
HEAD_DIM = 64
WINDOW = 128


NORM_EPS = 1e-06
CHANNEL_EPS = 1e-05
ROPE_BASE = 10000.0
MESH = pl.DeviceIdType.MESH

NY = 8
NZ = 8
WIN_COLS = 1792
WOUT_COLS = 1024
LAG = 4
RELS = (-3, -2, -1, 0, 1, 2, 3, 4)


def hops(first, a, b):
    main, side = (a, b) if first == 0 else (b, a)
    onward = []
    if side == 0:
        if 0 <= main < 4:
            onward.append((first, 1, main + 1, 0))
        if -3 < main <= 0:
            onward.append((first, -1, main - 1, 0))
    if 0 <= side < 4:
        onward.append((1 - first, 1, main, side + 1))
    if -3 < side <= 0:
        onward.append((1 - first, -1, main, side - 1))
    return [
        (axis, sign, m, s) if first == 0 else (axis, sign, s, m)
        for axis, sign, m, s in onward
    ]


def pieces_at(distance):
    found = [(a, b) for a in RELS for b in RELS if abs(a) + abs(b) == distance]
    return sorted(found, key=lambda ab: (min(abs(ab[0]), abs(ab[1])), ab))


def gather_kernel(win_ref, wout_ref, gin, gout, *sems):
    me = lax.axis_index("sp")
    core = lax.rem(me, 2)
    y = lax.rem(me // 2, NY)
    z = me // (2 * NY)
    ahead = 1 - 2 * core

    def device(zz, yy, cc):
        return {"sp": (zz * NY + yy) * 2 + cc}

    def near(axis, sign):
        step = sign * ahead
        if axis == 0:
            return device(lax.rem(z + step + NZ, NZ), y, core)
        return device(z, lax.rem(y + step + NY, NY), core)

    partner = device(z, y, 1 - core)
    neighbours = [near(0, 1), near(0, -1), near(1, 1), near(1, -1), partner]
    barrier = pltpu.get_barrier_semaphore()
    for one in neighbours:
        pl.semaphore_signal(barrier, inc=1, device_id=one, device_id_type=MESH)
    pl.semaphore_wait(barrier, len(neighbours))

    started = []

    def stage(own, full, recv, send, precv, psend, distance):
        cols = full.shape[-1] // 2
        for a, b in pieces_at(distance):
            oz = lax.rem(z - a * ahead + NZ, NZ)
            oy = lax.rem(y - b * ahead + NY, NY)
            slot = full.at[oz, oy, core]
            for first in range(2):
                part = (slice(None), pl.ds(first * cols, cols))
                source = own.at[part] if distance == 0 else slot.at[part]
                target = slot.at[part]
                if distance > 0:
                    pltpu.make_async_remote_copy(
                        src_ref=target,
                        dst_ref=target,
                        send_sem=send.at[first, 0, a + 3, b + 3],
                        recv_sem=recv.at[first, a + 3, b + 3],
                        device_id=near(0, 1),
                        device_id_type=MESH,
                    ).wait_recv()
                for way, (axis, sign, a2, b2) in enumerate(hops(first, a, b)):
                    copy = pltpu.make_async_remote_copy(
                        src_ref=source,
                        dst_ref=target,
                        send_sem=send.at[first, way, a + 3, b + 3],
                        recv_sem=recv.at[first, a2 + 3, b2 + 3],
                        device_id=near(axis, sign),
                        device_id_type=MESH,
                    )
                    copy.start()
                    started.append(copy)
            copy = pltpu.make_async_remote_copy(
                src_ref=own if distance == 0 else slot,
                dst_ref=slot,
                send_sem=psend.at[a + 3, b + 3],
                recv_sem=precv.at[a + 3, b + 3],
                device_id=partner,
                device_id_type=MESH,
            )
            copy.start()
            started.append(copy)

    def from_partner(full, precv, psend):
        for a in RELS:
            for b in RELS:
                oz = lax.rem(z + a * ahead + NZ, NZ)
                oy = lax.rem(y + b * ahead + NY, NY)
                slot = full.at[oz, oy, 1 - core]
                pltpu.make_async_remote_copy(
                    src_ref=slot,
                    dst_ref=slot,
                    send_sem=psend.at[a + 3, b + 3],
                    recv_sem=precv.at[a + 3, b + 3],
                    device_id=partner,
                    device_id_type=MESH,
                ).wait_recv()

    for tick in range(9 + LAG):
        if tick < 9:
            stage(win_ref, gin, *sems[:4], tick)
        if tick == 0:
            gin[z, y, core] = win_ref[...]
            gout[z, y, core] = wout_ref[...]
        if tick >= LAG:
            stage(wout_ref, gout, *sems[4:], tick - LAG)
    from_partner(gin, *sems[2:4])
    from_partner(gout, *sems[6:8])
    for copy in started:
        copy.wait_send()


def gathered(win, wout):
    dma = pltpu.SemaphoreType.DMA
    one = [dma((2, 8, 8)), dma((2, 4, 8, 8)), dma((8, 8)), dma((8, 8))]
    vmem = pl.BlockSpec(memory_space=pltpu.VMEM)
    gin, gout = pl.pallas_call(
        gather_kernel,
        out_shape=(
            jax.ShapeDtypeStruct((NZ, NY, 2, 16, WIN_COLS), jnp.bfloat16),
            jax.ShapeDtypeStruct((NZ, NY, 2, 16, WOUT_COLS), jnp.bfloat16),
        ),
        in_specs=[vmem, vmem],
        out_specs=(vmem, vmem),
        scratch_shapes=one + one,
        compiler_params=pltpu.CompilerParams(collective_id=0, has_side_effects=True),
        name="gather_weights",
    )(win, wout)
    return gin.reshape(2048, WIN_COLS), gout.reshape(2048, WOUT_COLS)


def sent_together(arrays, axis, dim, along):
    widths = [a.shape[along] for a in arrays]
    both = jnp.concatenate(arrays, axis=along)
    whole = lax.all_gather(both, axis, axis=dim, tiled=True)
    return tuple(jnp.split(whole, [sum(widths[:k]) for k in range(1, len(widths))], axis=along))


def shifted(value, axis, steps):
    count = lax.axis_size(axis)
    initial, last = (max(0, -steps), min(count, count - steps))
    return lax.ppermute(value, axis, [(source, source + steps) for source in range(initial, last)])


def from_everyone(shard, axis):
    peers = lax.axis_size(axis)
    return lax.all_to_all(
        jnp.broadcast_to(shard[None], (peers, *shard.shape)), axis, 0, 0, tiled=True
    )


def taken_together(shard, axis):
    everything = from_everyone(shard, axis)
    return jnp.sum(everything, axis=0)


def packed_total(arrays, axis):
    ravelled, at, finished = (jnp.concatenate([a.reshape(-1) for a in arrays]), 0, [])
    subtotal = taken_together(ravelled, axis)
    for a in arrays:
        finished.append(subtotal[at : at + a.size].reshape(a.shape))
        at += a.size
    return tuple(finished)


def turned_gather(arrays, axis, dims):
    turned = [jnp.moveaxis(a, dim, 0) for a, dim in zip(arrays, dims)]
    both = jnp.concatenate([t.reshape(len(t), -1) for t in turned], axis=1)
    whole, at, finished = (lax.all_gather(both, axis, axis=0, tiled=True), 0, [])
    for t, dim in zip(turned, dims):
        piece = whole[:, at : at + t[0].size].reshape(-1, *t.shape[1:])
        finished.append(jnp.moveaxis(piece, 0, dim))
        at += t[0].size
    return tuple(finished)


def cut_along(shard, dim, peers):
    dims = shard.shape
    pieces = shard.reshape(*dims[:dim], peers, dims[dim] // peers, *dims[dim + 1 :])
    return jnp.moveaxis(pieces, dim, 0)


def summed_on_arrival(shard, axis, dim):
    pieces = cut_along(shard, dim, lax.axis_size(axis))
    arrived = lax.all_to_all(pieces, axis, split_axis=0, concat_axis=0, tiled=True)
    return arrived.astype(jnp.float32).sum(axis=0)


def rotate(heads, positions):
    half_dim = heads.shape[-1] // 2
    inverse = ROPE_BASE ** (-jnp.arange(half_dim, dtype=jnp.float32) / half_dim)
    angles = positions.astype(jnp.float32)[:, None] * inverse[None, :]
    cosine = jnp.cos(angles)[:, None, :]
    sine = jnp.sin(angles)[:, None, :]
    as_float = heads.astype(jnp.float32)
    front_part = as_float[..., :half_dim]
    back_part = as_float[..., half_dim:]
    return jnp.concatenate(
        [front_part * cosine - back_part * sine, back_part * cosine + front_part * sine], axis=-1
    )


def shards(
    tokens,
    norm_gain,
    w_conv_value,
    w_conv_gate,
    w_query,
    w_key,
    w_value,
    conv_taps,
    ln_gain,
    sinks,
    out_conv,
    out_attn,
):
    as_float = tokens.astype(jnp.float32)
    normed = (
        as_float
        * lax.rsqrt(jnp.mean(as_float * as_float, axis=-1, keepdims=True) + NORM_EPS)
        * norm_gain.astype(jnp.float32)
    ).astype(jnp.bfloat16)
    row_count = normed.shape[0]
    win, wout = gathered(
        jnp.concatenate([w_conv_value, w_conv_gate, w_query, w_key, w_value], axis=1),
        jnp.concatenate([out_conv.T, out_attn.T], axis=1),
    )
    pieces = jnp.split(win, (512, 1024, 1536, 1664), axis=1)
    projected = tuple(
        (jnp.dot(normed, piece, preferred_element_type=jnp.float32) for piece in pieces)
    )
    conv_value, conv_gate, query_raw, key_raw, value_rows = [
        item.astype(jnp.bfloat16) for item in projected
    ]
    glu = (conv_value.astype(jnp.float32) * jax.nn.sigmoid(conv_gate.astype(jnp.float32))).astype(
        jnp.bfloat16
    )
    offset = lax.axis_index("sp") * row_count
    positions = offset + jnp.arange(row_count, dtype=jnp.int32)
    query_heads = query_raw.shape[1] // HEAD_DIM
    key_heads = key_raw.shape[1] // HEAD_DIM
    query = rotate(query_raw.reshape(row_count, query_heads, HEAD_DIM), positions).astype(
        jnp.bfloat16
    )
    key = rotate(key_raw.reshape(row_count, key_heads, HEAD_DIM), positions).astype(jnp.bfloat16)
    reach = conv_taps.shape[0] - 1
    key_tail = key[row_count - WINDOW :]
    value_tail = value_rows.reshape(row_count, key_heads, HEAD_DIM)[row_count - WINDOW :]
    glu_tail = glu[row_count - reach :]
    glu_before = shifted(glu_tail, "sp", 1)
    key_before, value_before = shifted((key_tail, value_tail), "sp", 1)
    extended = jnp.concatenate([glu_before, glu], axis=0).astype(jnp.float32)
    conv_out = jnp.zeros((row_count, glu.shape[1]), jnp.float32)
    for tap in range(reach + 1):
        conv_out = conv_out + conv_taps[tap][None, :] * extended[tap : tap + row_count]
    sum_first = jnp.sum(conv_out, axis=-1)
    sum_second = jnp.sum(conv_out * conv_out, axis=-1)
    total_first, total_second = packed_total((sum_first, sum_second), "tp")
    mean = (total_first / CONV_CH)[:, None]
    var = (total_second / CONV_CH)[:, None] - mean * mean
    conv_branch = jax.nn.silu(
        (conv_out - mean) * lax.rsqrt(var + CHANNEL_EPS) * ln_gain[None, :]
    ).astype(jnp.bfloat16)
    group = HEADS // KV_HEADS
    blocks = row_count // WINDOW
    q_blocks = query.reshape(blocks, WINDOW, key_heads, group, HEAD_DIM)
    key_blocks = jnp.concatenate([key_before, key], axis=0).reshape(
        blocks + 1, WINDOW, key_heads, HEAD_DIM
    )
    value_all = jnp.concatenate(
        [value_before, value_rows.reshape(row_count, key_heads, HEAD_DIM)], axis=0
    )
    value_blocks = value_all.reshape(blocks + 1, WINDOW, key_heads, HEAD_DIM)
    key_window = jnp.concatenate([key_blocks[:-1], key_blocks[1:]], axis=1)
    value_window = jnp.concatenate([value_blocks[:-1], value_blocks[1:]], axis=1)
    scores = jnp.einsum(
        "nqhgd,nkhd->nhgqk", q_blocks, key_window, preferred_element_type=jnp.float32
    ) * HEAD_DIM ** (-0.5)
    query_index = jnp.arange(WINDOW)[:, None] + WINDOW
    key_index = jnp.arange(2 * WINDOW)[None, :]
    band = (key_index <= query_index) & (query_index - key_index < WINDOW)
    block_index = jnp.arange(blocks)[:, None, None]
    allowed = band[None] & (offset + block_index * WINDOW + key_index[None] - WINDOW >= 0)
    allowed = allowed[:, None, None]
    totals = jnp.sum(jnp.where(allowed, jnp.exp(scores), 0.0), axis=-1)
    totals = totals + jnp.exp(sinks).reshape(1, key_heads, group, 1)
    log_total = jnp.log(totals)
    weights = jnp.where(allowed, jnp.exp(scores - log_total[..., None]), 0.0).astype(jnp.bfloat16)
    attended = jnp.einsum(
        "nhgqk,nkhd->nqhgd", weights, value_window, preferred_element_type=jnp.float32
    )
    attn_branch = attended.astype(jnp.bfloat16).reshape(row_count, query_heads * HEAD_DIM)
    log_sums = log_total.transpose(1, 2, 0, 3).reshape(query_heads, row_count)
    mixed = summed_on_arrival(
        (
            jnp.dot(conv_branch, wout[:, :512].T, preferred_element_type=jnp.float32)
            + jnp.dot(attn_branch, wout[:, 512:].T, preferred_element_type=jnp.float32)
        ).astype(jnp.bfloat16),
        "tp",
        0,
    )
    return (mixed.astype(jnp.bfloat16), log_sums)


def solution(mesh):
    in_specs = (
        P("sp", None),
        P(),
        P("sp", "tp"),
        P("sp", "tp"),
        P("sp", "tp"),
        P("sp", "tp"),
        P("sp", "tp"),
        P(None, "tp"),
        P("tp"),
        P("tp"),
        P("tp", "sp"),
        P("tp", "sp"),
    )
    out_specs = (P(("sp", "tp"), None), P("tp", "sp"))
    return jax.shard_map(shards, mesh=mesh, in_specs=in_specs, out_specs=out_specs, check_vma=False)
```

```python
import jax
import jax.numpy as jnp
from jax import lax
from jax.experimental import pallas as pl
from jax.experimental.pallas import tpu as pltpu
from jax.sharding import PartitionSpec as P

CONV_CH = 2048
HEADS = 32
KV_HEADS = 8
HEAD_DIM = 64
WINDOW = 128
NORM_EPS = 1e-06
CHANNEL_EPS = 1e-05
ROPE_BASE = 10000.0
MESH = pl.DeviceIdType.MESH
F32 = jnp.float32
BF16 = jnp.bfloat16

SIDE = 8
TP = 4
ROWS = 512
WIDTH = 2048
GROUPS = ((0, 1792), (1792, 2816))
ORDER = (0, 1, -1, 2, -2, 3, -3, 4)
NT = (((1,), (1,)), ((), ()))


def kernel(
    tokens_ref,
    gain_ref,
    wcv_ref,
    wcg_ref,
    wq_ref,
    wk_ref,
    wv_ref,
    taps_ref,
    lng_ref,
    sinks_ref,
    oc_ref,
    oa_ref,
    cos_ref,
    sin_ref,
    mixed_ref,
    logs_ref,
    full,
    piece,
    tok,
    normed,
    raw,
    ext,
    conv,
    sums,
    q_buf,
    kz,
    vz,
    act,
    halo_send,
    halo_recv,
    glu_send,
    glu_recv,
    stat_send,
    stat_recv,
    part,
    relay_in,
    relay_out,
    from_low,
    from_high,
    tok_sem,
    drecv,
    dsend,
    rrecv,
    rsend,
    precv,
    psend,
    hsend,
    hrecv,
    ssend,
    srecv,
    xsend,
    xrecv,
):
    me = lax.axis_index("sp")
    x = lax.axis_index("tp")
    core = lax.rem(me, 2)
    y = lax.rem(me // 2, SIDE)
    z = me // (2 * SIDE)

    def device(zz, yy, cc):
        return {"sp": (zz * SIDE + yy) * 2 + cc}

    def wrap(v):
        return lax.rem(v + 2 * SIDE, SIDE)

    def at(a, b, c):
        return wrap(z + (1 - c) * a + c * b), wrap(y + (1 - c) * b + c * a)

    def peer(a, b):
        return device(*at(a, b, core), core)

    def across(d):
        return {"tp": lax.rem(x + d + TP, TP)}

    partner = device(z, y, 1 - core)
    count = 2 * SIDE * SIDE
    after = {"sp": lax.rem(me + 1, count)}
    before = {"sp": lax.rem(me + count - 1, count)}
    started = []

    def remote(src, dst, send, recv, to):
        return pltpu.make_async_remote_copy(
            src_ref=src,
            dst_ref=dst,
            send_sem=send,
            recv_sem=recv,
            device_id=to,
            device_id_type=MESH,
        )

    def go(src, dst, send, recv, to):
        copy = remote(src, dst, send, recv, to)
        copy.start()
        started.append(copy)

    tok_copy = pltpu.make_async_copy(tokens_ref, tok, tok_sem)
    tok_copy.start()
    piece[:, 0:512] = wcv_ref[...]
    piece[:, 512:1024] = wcg_ref[...]
    piece[:, 1024:1536] = wq_ref[...]
    piece[:, 1536:1664] = wk_ref[...]
    piece[:, 1664:1792] = wv_ref[...]
    piece[:, 1792:2304] = oc_ref[...]
    piece[:, 2304:2816] = oa_ref[...]
    full[pl.ds(pl.multiple_of(me * 16, 16), 16), :] = piece[...]

    greeted = [peer(a, 0) for a in ORDER[1:]] + [peer(0, 1), peer(0, -1), partner]
    greeted += [after, before] + [across(d) for d in (1, 2, 3)]
    barrier = pltpu.get_barrier_semaphore()
    for one in greeted:
        pl.semaphore_signal(barrier, inc=1, device_id=one, device_id_type=MESH)
    pl.semaphore_wait(barrier, len(greeted))

    def slot(g, a, b, c=None, half=None):
        c = core if c is None else c
        zz, yy = at(-a, -b, c)
        low, high = GROUPS[g]
        width = high - low
        if half is not None:
            width = width // 2
            low = low + half * width
        row = pl.multiple_of(((zz * SIDE + yy) * 2 + c) * 16, 16)
        return full.at[pl.ds(row, 16), pl.ds(low, width)]

    def own(g):
        low, high = GROUPS[g]
        return piece.at[:, pl.ds(low, high - low)]

    def direct(g):
        for i, a in enumerate(ORDER):
            if a:
                go(own(g), slot(g, 0, 0), dsend.at[g, i], drecv.at[g, i], peer(a, 0))

    def arrived(ref, sem):
        remote(ref, ref, hsend.at[0], sem, partner).wait_recv()

    def to_partner(g, i, a, b):
        ref = slot(g, a, b)
        go(own(g) if a == b == 0 else ref, ref, psend.at[g, i, b + 3], precv.at[g, i, b + 3], partner)

    def batch(g, s):
        for i, a in enumerate(ORDER):
            if s == 0:
                ref = slot(g, a, 0)
                if a:
                    arrived(ref, drecv.at[g, i])
                src = ref if a else own(g)
                go(src, ref, rsend.at[g, i, 3], rrecv.at[g, i, 4], peer(0, 1))
                go(src, ref, rsend.at[g, i, 4], rrecv.at[g, i, 2], peer(0, -1))
                to_partner(g, i, a, 0)
            elif s < 4:
                for sign in (1, -1):
                    ref = slot(g, a, sign * s)
                    arrived(ref, rrecv.at[g, i, 3 + sign * s])
                    if s < 3:
                        b = sign * (s + 1)
                        lane = 4 + s if sign > 0 else 3 - s
                        go(ref, ref, rsend.at[g, i, lane], rrecv.at[g, i, 3 + b], peer(0, sign))
                    else:
                        h = 0 if sign > 0 else 1
                        ref = slot(g, a, sign * s, half=h)
                        lane = 7 if sign > 0 else 0
                        go(ref, ref, rsend.at[g, i, lane], rrecv.at[g, i, 7 + h], peer(0, sign))
                    to_partner(g, i, a, sign * s)
            else:
                for h in range(2):
                    arrived(slot(g, a, 4, half=h), rrecv.at[g, i, 7 + h])
                to_partner(g, i, a, 4)

    def from_partner(g):
        for i, a in enumerate(ORDER):
            for b in ORDER:
                arrived(slot(g, a, b, 1 - core), precv.at[g, i, b + 3])

    def norm_rows(t, carry):
        rows = pl.ds(pl.multiple_of(t * 32, 32), 32)
        v = tok[rows, :].astype(F32)
        scale = lax.rsqrt(jnp.mean(v * v, axis=-1, keepdims=True) + NORM_EPS)
        normed[rows, :] = (v * scale * gain_ref[...].astype(F32)).astype(BF16)
        return carry

    def project(t, carry):
        cols = pl.ds(pl.multiple_of(t * 256, 256), 256)
        raw[:, cols] = jnp.dot(
            normed[...], full[:, cols], preferred_element_type=F32
        ).astype(BF16)
        return carry

    def glu_rows(t, carry):
        rows = pl.ds(pl.multiple_of(t * 64, 64), 64)
        into = pl.ds(pl.multiple_of(32 + t * 64, 32), 64)
        for c in range(4):
            value = raw[rows, c * 128 : (c + 1) * 128].astype(F32)
            gate = raw[rows, 512 + c * 128 : 640 + c * 128].astype(F32)
            glu = value * jax.nn.sigmoid(gate)
            ext[c, into, :] = glu.astype(BF16).astype(F32)
        return carry

    lane = lax.broadcasted_iota(jnp.int32, (64, 128), 1)
    low_part = lax.rem(lane, 64) < 32

    def rotated(v, rows):
        other = jnp.where(low_part, pltpu.roll(v, 96, 1), pltpu.roll(v, 32, 1))
        return v * cos_ref[rows, :] + other * sin_ref[rows, :]

    def spread(buf, v, into, wide):
        first = jnp.where(wide < 64, v, 0.0)
        second = jnp.where(wide < 64, 0.0, v)
        buf[0, into, :] = first.astype(BF16)
        buf[1, into, :] = pltpu.roll(first, 64, 1).astype(BF16)
        buf[2, into, :] = pltpu.roll(second, 64, 1).astype(BF16)
        buf[3, into, :] = second.astype(BF16)

    def key_rows(t, carry):
        rows = pl.ds(pl.multiple_of(t * 64, 64), 64)
        into = pl.ds(pl.multiple_of(128 + t * 64, 64), 64)
        key = rotated(raw[rows, 1536:1664].astype(F32), rows).astype(BF16)
        spread(kz, key.astype(F32), into, lane)
        spread(vz, raw[rows, 1664:1792].astype(F32), into, lane)
        keep = pl.ds(pl.multiple_of(t * 64, 64), 64)
        halo_send[0, keep, :] = key
        return carry

    def query_rows(t, carry):
        rows = pl.ds(pl.multiple_of(t * 64, 64), 64)
        for c in range(4):
            cols = slice(1024 + c * 128, 1152 + c * 128)
            turned = rotated(raw[rows, cols].astype(F32), rows)
            q_buf[rows, c * 128 : (c + 1) * 128] = (turned * HEAD_DIM**-0.5).astype(BF16)
        return carry

    def conv_rows(t, carry):
        rows = pl.ds(pl.multiple_of(t * 64, 64), 64)
        first = jnp.zeros((64, 128), F32)
        second = jnp.zeros((64, 128), F32)
        for c in range(4):
            near = ext[c, pl.ds(pl.multiple_of(t * 64, 64), 96), :]
            total = None
            for shift in range(8):
                acc = None
                span = 72 if shift else 64
                for whole in range(0, 40, 8):
                    tap = whole + shift - 2
                    if 0 <= tap < 31:
                        term = taps_ref[tap : tap + 1, c * 128 : (c + 1) * 128] * near[whole : whole + span]
                        acc = term if acc is None else acc + term
                acc = acc[shift : shift + 64]
                total = acc if total is None else total + acc
            conv[c, rows, :] = total
            first = first + total
            second = second + total * total
        sums[0, rows, :] = first
        sums[1, rows, :] = second
        return carry

    def branch_rows(t, carry):
        rows = pl.ds(pl.multiple_of(t * 64, 64), 64)
        mean = sums[0, rows, :]
        scale = sums[1, rows, :]
        for c in range(4):
            cols = slice(c * 128, (c + 1) * 128)
            v = (conv[c, rows, :] - mean) * scale * lng_ref[0:1, cols]
            act[rows, cols] = (v * jax.nn.sigmoid(v)).astype(BF16)
        return carry

    seen = lax.broadcasted_iota(jnp.int32, (128, 256), 1)
    asks = lax.broadcasted_iota(jnp.int32, (128, 256), 0)
    head_lane = lax.broadcasted_iota(jnp.int32, (128, 128), 1)

    def attend(t, carry):
        rows = pl.ds(pl.multiple_of(t * 128, 128), 128)
        window = pl.ds(pl.multiple_of(t * 128, 128), 256)
        least = jnp.where(me * SIDE + t == 0, WINDOW, 0)
        allowed = (seen > asks) & (seen <= asks + WINDOW) & (seen >= least)
        logs = jnp.zeros((128, 128), F32)
        for pair in range(4):
            q = q_buf[rows, pair * 128 : (pair + 1) * 128]
            out = None
            for odd in range(2):
                head = 2 * pair + odd
                which = 2 * (pair // 2) + odd
                scores = lax.dot_general(q, kz[which, window, :], NT, preferred_element_type=F32)
                weight = jnp.where(allowed, jnp.exp(scores), 0.0)
                total = jnp.sum(weight, axis=1, keepdims=True)
                total = total + jnp.exp(sinks_ref[0:1, head : head + 1])
                logs = jnp.where(head_lane == head, jnp.log(total), logs)
                weight = (weight * (1.0 / total)).astype(BF16)
                term = jnp.dot(weight, vz[which, window, :], preferred_element_type=F32)
                out = term if out is None else out + term
            act[rows, 512 + pair * 128 : 640 + pair * 128] = out.astype(BF16)
        sums[2, rows, :] = logs
        return carry

    direct(0)
    direct(1)
    tok_copy.wait()
    batch(0, 0)
    lax.fori_loop(0, 6, norm_rows, 0)
    batch(0, 1)
    lax.fori_loop(6, 12, norm_rows, 0)
    batch(0, 2)
    lax.fori_loop(12, 16, norm_rows, 0)
    batch(0, 3)
    batch(1, 0)
    batch(0, 4)
    batch(1, 1)
    from_partner(0)

    lax.fori_loop(0, 4, project, 0)
    batch(1, 2)
    lax.fori_loop(0, 8, glu_rows, 0)
    for c in range(4):
        glu_send[:, c * 128 : (c + 1) * 128] = ext[c, 512:544, :].astype(BF16)
    lax.fori_loop(4, 7, project, 0)
    go(glu_send, glu_recv, hsend.at[0], hrecv.at[0], after)
    batch(1, 3)
    lax.fori_loop(0, 8, key_rows, 0)
    halo_send[1, 384:512, :] = raw[384:512, 1664:1792]
    lax.fori_loop(0, 8, query_rows, 0)
    tail = pl.ds(384, 128)
    go(halo_send.at[0, tail], halo_recv.at[0], hsend.at[1], hrecv.at[1], after)
    go(halo_send.at[1, tail], halo_recv.at[1], hsend.at[2], hrecv.at[2], after)
    batch(1, 4)
    arrived(glu_recv, hrecv.at[0])
    keep = jnp.where(me == 0, 0.0, 1.0).astype(F32)
    for c in range(4):
        ext[c, 0:32, :] = glu_recv[:, c * 128 : (c + 1) * 128].astype(F32) * keep
    lax.fori_loop(0, 8, conv_rows, 0)
    stat_send[...] = jnp.zeros((8, ROWS), F32)
    stat_send[0:1, :] = jnp.sum(sums[0].T, axis=0, keepdims=True)
    stat_send[1:2, :] = jnp.sum(sums[1].T, axis=0, keepdims=True)
    for d in (1, 2, 3):
        go(stat_send, stat_recv.at[d - 1], ssend.at[d - 1], srecv.at[d - 1], across(d))
    arrived(halo_recv.at[0], hrecv.at[1])
    arrived(halo_recv.at[1], hrecv.at[2])
    for t in range(2):
        rows = slice(t * 64, t * 64 + 64)
        spread(kz, halo_recv[0, rows, :].astype(F32), rows, lane)
        spread(vz, halo_recv[1, rows, :].astype(F32), rows, lane)
    lax.fori_loop(0, 4, attend, 0)
    logs_ref[...] = sums[2].T[0:8, :]
    for d in range(3):
        arrived(stat_recv.at[d], srecv.at[d])
    stats = stat_send[0:2, :] + stat_recv[0, 0:2, :] + stat_recv[1, 0:2, :] + stat_recv[2, 0:2, :]
    stats = stats / CONV_CH
    mean = stats[0:1, :]
    scale = lax.rsqrt(stats[1:2, :] - mean * mean + CHANNEL_EPS)
    sums[0] = jnp.broadcast_to(mean, (128, ROWS)).T
    sums[1] = jnp.broadcast_to(scale, (128, ROWS)).T
    lax.fori_loop(0, 8, branch_rows, 0)
    from_partner(1)

    def rows_of(d):
        return pl.ds(pl.multiple_of(lax.rem(x + d + TP, TP) * 128, 128), 128)

    def out_part(n):
        def one(t, carry):
            cols = pl.ds(pl.multiple_of(t * 256, 256), 256)
            wrows = pl.ds(pl.multiple_of(n * 512 + t * 256, 256), 256)
            part[n, :, cols] = lax.dot_general(
                act[...], full[wrows, 1792:2816], NT, preferred_element_type=F32
            ).astype(BF16)
            return carry

        lax.fori_loop(0, 2, one, 0)

    inbox = {1: from_low, -1: from_high}
    for n in (0, 2, 1, 3):
        out_part(n)
        far = 1 if n < 2 else -1
        go(part.at[n, rows_of(2)], relay_in.at[n], xsend.at[0, n], xrecv.at[0, n], across(far))
        go(part.at[n, rows_of(-far)], inbox[-far].at[n], xsend.at[1, n], xrecv.at[1, n], across(-far))
    for n in (0, 2, 1, 3):
        far = 1 if n < 2 else -1
        arrived(relay_in.at[n], xrecv.at[0, n])
        relay_out[n] = (
            part[n, rows_of(far), :].astype(F32) + relay_in[n].astype(F32)
        ).astype(BF16)
        go(relay_out.at[n], inbox[far].at[n], xsend.at[2, n], xrecv.at[2, n], across(far))
    for n in (0, 2, 1, 3):
        arrived(from_low.at[n], xrecv.at[2 if n < 2 else 1, n])
        arrived(from_high.at[n], xrecv.at[1 if n < 2 else 2, n])
        mixed_ref[:, n * 512 : (n + 1) * 512] = (
            part[n, rows_of(0), :].astype(F32)
            + from_low[n].astype(F32)
            + from_high[n].astype(F32)
        ).astype(BF16)
    for copy in started:
        copy.wait_send()


def shards(
    tokens,
    norm_gain,
    w_conv_value,
    w_conv_gate,
    w_query,
    w_key,
    w_value,
    conv_taps,
    ln_gain,
    sinks,
    out_conv,
    out_attn,
):
    half_dim = HEAD_DIM // 2
    position = lax.axis_index("sp") * ROWS + lax.broadcasted_iota(jnp.int32, (ROWS, 128), 0)
    which = lax.broadcasted_iota(jnp.int32, (ROWS, 128), 1)
    inverse = ROPE_BASE ** (-(which % half_dim).astype(F32) / half_dim)
    angles = position.astype(F32) * inverse
    cosine = jnp.cos(angles)
    sine = jnp.where(which % HEAD_DIM < half_dim, -1.0, 1.0) * jnp.sin(angles)
    dma = pltpu.SemaphoreType.DMA
    vmem = pl.BlockSpec(memory_space=pltpu.VMEM)
    V = pltpu.VMEM
    return pl.pallas_call(
        kernel,
        out_shape=(
            jax.ShapeDtypeStruct((128, WIDTH), BF16),
            jax.ShapeDtypeStruct((8, ROWS), F32),
        ),
        in_specs=[pl.BlockSpec(memory_space=pl.ANY)] + [vmem] * 13,
        out_specs=(vmem, vmem),
        scratch_shapes=[
            V((WIDTH, 2816), BF16),
            V((16, 2816), BF16),
            V((ROWS, WIDTH), BF16),
            V((ROWS, WIDTH), BF16),
            V((ROWS, 1792), BF16),
            V((4, 544, 128), F32),
            V((4, ROWS, 128), F32),
            V((3, ROWS, 128), F32),
            V((ROWS, 512), BF16),
            V((4, 640, 128), BF16),
            V((4, 640, 128), BF16),
            V((ROWS, 1024), BF16),
            V((2, ROWS, 128), BF16),
            V((2, 128, 128), BF16),
            V((32, 512), BF16),
            V((32, 512), BF16),
            V((8, ROWS), F32),
            V((3, 8, ROWS), F32),
            V((4, ROWS, 512), BF16),
            V((4, 128, 512), BF16),
            V((4, 128, 512), BF16),
            V((4, 128, 512), BF16),
            V((4, 128, 512), BF16),
            dma,
            dma((2, 8)),
            dma((2, 8)),
            dma((2, 8, 9)),
            dma((2, 8, 8)),
            dma((2, 8, 8)),
            dma((2, 8, 8)),
            dma((3,)),
            dma((3,)),
            dma((3,)),
            dma((3,)),
            dma((3, 4)),
            dma((3, 4)),
        ],
        compiler_params=pltpu.CompilerParams(collective_id=0, has_side_effects=True),
        name="layer",
    )(
        tokens,
        norm_gain.reshape(1, WIDTH),
        w_conv_value,
        w_conv_gate,
        w_query,
        w_key,
        w_value,
        conv_taps,
        ln_gain.reshape(1, 512),
        sinks.reshape(1, 8),
        out_conv.T,
        out_attn.T,
        cosine,
        sine,
    )


def solution(mesh):
    in_specs = (
        P("sp", None),
        P(),
        P("sp", "tp"),
        P("sp", "tp"),
        P("sp", "tp"),
        P("sp", "tp"),
        P("sp", "tp"),
        P(None, "tp"),
        P("tp"),
        P("tp"),
        P("tp", "sp"),
        P("tp", "sp"),
    )
    out_specs = (P(("sp", "tp"), None), P("tp", "sp"))
    return jax.shard_map(shards, mesh=mesh, in_specs=in_specs, out_specs=out_specs, check_vma=False)
```

```python
import jax
import jax.numpy as jnp
import numpy as np
from jax import lax
from jax.experimental import pallas as pl
from jax.experimental.pallas import tpu as pltpu
from jax.sharding import PartitionSpec as P

CONV_CH = 2048
HEADS = 32
KV_HEADS = 8
HEAD_DIM = 64
WINDOW = 128
NORM_EPS = 1e-06
CHANNEL_EPS = 1e-05
ROPE_BASE = 10000.0
MESH = pl.DeviceIdType.MESH
F32 = jnp.float32
BF16 = jnp.bfloat16

SIDE = 8
TP = 4
ROWS = 512
WIDTH = 2048
GROUPS = ((0, 1024), (1024, 1792), (1792, 2816))
ORDER = (0, 1, -1, 2, -2, 3, -3, 4)
NT = (((1,), (1,)), ((), ()))


def kernel(
    tokens_ref,
    gain_ref,
    wcv_ref,
    wcg_ref,
    wq_ref,
    wk_ref,
    wv_ref,
    taps_ref,
    lng_ref,
    sinks_ref,
    oc_ref,
    oa_ref,
    inv_ref,
    mixed_ref,
    logs_ref,
    full,
    piece,
    tok,
    normed,
    raw,
    ext,
    conv,
    sums,
    q_buf,
    kz,
    vz,
    act,
    halo_send,
    halo_recv,
    glu_send,
    glu_recv,
    stat_send,
    stat_recv,
    part,
    relay_in,
    relay_out,
    from_low,
    from_high,
    tok_sem,
    drecv,
    rrecv,
    precv,
    gsend,
    hsend,
    hrecv,
    ssend,
    srecv,
    xsend,
    xrecv,
    cos_ref,
    sin_ref,
):
    me = lax.axis_index("sp")
    x = lax.axis_index("tp")
    core = lax.rem(me, 2)
    y = lax.rem(me // 2, SIDE)
    z = me // (2 * SIDE)

    def device(zz, yy, cc):
        return {"sp": (zz * SIDE + yy) * 2 + cc}

    def wrap(v):
        return lax.rem(v + 2 * SIDE, SIDE)

    def at(a, b, c):
        return wrap(z + (1 - c) * a + c * b), wrap(y + (1 - c) * b + c * a)

    def peer(a, b):
        return device(*at(a, b, core), core)

    def across(d):
        return {"tp": lax.rem(x + d + TP, TP)}

    partner = device(z, y, 1 - core)
    count = 2 * SIDE * SIDE
    after = {"sp": lax.rem(me + 1, count)}
    before = {"sp": lax.rem(me + count - 1, count)}
    started = []

    def remote(src, dst, send, recv, to):
        return pltpu.make_async_remote_copy(
            src_ref=src,
            dst_ref=dst,
            send_sem=send,
            recv_sem=recv,
            device_id=to,
            device_id_type=MESH,
        )

    def go(src, dst, send, recv, to):
        copy = remote(src, dst, send, recv, to)
        copy.start()
        started.append(copy)

    tok_copy = pltpu.make_async_copy(tokens_ref, tok, tok_sem)
    tok_copy.start()
    piece[:, 0:512] = wcv_ref[...]
    piece[:, 512:1024] = wcg_ref[...]
    piece[:, 1024:1536] = wq_ref[...]
    piece[:, 1536:1664] = wk_ref[...]
    piece[:, 1664:1792] = wv_ref[...]
    piece[:, 1792:2304] = oc_ref[...]
    piece[:, 2304:2816] = oa_ref[...]
    full[pl.ds(pl.multiple_of(me * 16, 16), 16), :] = piece[...]

    greeted = [peer(a, 0) for a in ORDER[1:]] + [peer(0, 1), peer(0, -1), partner]
    greeted += [after, before] + [across(d) for d in (1, 2, 3)]
    barrier = pltpu.get_barrier_semaphore()
    for one in greeted:
        pl.semaphore_signal(barrier, inc=1, device_id=one, device_id_type=MESH)
    pl.semaphore_wait(barrier, len(greeted))

    def slot(g, a, b, c=None, half=None):
        c = core if c is None else c
        zz, yy = at(-a, -b, c)
        low, high = GROUPS[g]
        width = high - low
        if half is not None:
            width = width // 2
            low = low + half * width
        row = pl.multiple_of(((zz * SIDE + yy) * 2 + c) * 16, 16)
        return full.at[pl.ds(row, 16), pl.ds(low, width)]

    def own(g):
        low, high = GROUPS[g]
        return piece.at[:, pl.ds(low, high - low)]

    def direct(g):
        for i, a in enumerate(ORDER):
            if a:
                remote(own(g), slot(g, 0, 0), gsend.at[g], drecv.at[g, i], peer(a, 0)).start()

    def arrived(ref, sem):
        remote(ref, ref, hsend.at[0], sem, partner).wait_recv()

    def place(i):
        if isinstance(i, int):
            return ORDER[i]
        return (i + 1) // 2 * (2 * lax.rem(i, 2) - 1)

    def serve(g, s, i):
        a = place(i)

        def ring(src, ref, b, recv):
            remote(src, ref, gsend.at[g], recv, peer(0, 1 if b > 0 else -1)).start()

        def share(src, ref):
            remote(src, ref, gsend.at[g], precv.at[g], partner).start()

        if s == 0:
            ref = slot(g, a, 0)
            if a:
                arrived(ref, drecv.at[g, i])
            src = ref if a else own(g)
            for b in (1, -1):
                ring(src, ref, b, rrecv.at[g, i, 3 + b])
            share(src, ref)
        elif s < 4:
            for sign in (1, -1):
                ref = slot(g, a, sign * s)
                arrived(ref, rrecv.at[g, i, 3 + sign * s])
                if s < 3:
                    b = sign * (s + 1)
                    ring(ref, ref, b, rrecv.at[g, i, 3 + b])
                else:
                    h = 0 if sign > 0 else 1
                    out = slot(g, a, sign * s, half=h)
                    ring(out, out, sign, rrecv.at[g, i, 7 + h])
                share(ref, ref)
        else:
            for h in range(2):
                arrived(slot(g, a, 4, half=h), rrecv.at[g, i, 7 + h])
            share(slot(g, a, 4), slot(g, a, 4))

    def batch(g, s, items=range(8)):
        for i in items:
            serve(g, s, i)

    def rows_in(g, count):
        low, high = GROUPS[g]
        return full.at[pl.ds(0, count), pl.ds(low, high - low)]

    def from_partner(g):
        arrived(rows_in(g, 1024), precv.at[g])

    def sent(g):
        ref = rows_in(g, 127 * 16)
        remote(ref, ref, gsend.at[g], tok_sem, partner).wait_send()

    def norm_rows(t, carry):
        rows = pl.ds(pl.multiple_of(t * 32, 32), 32)
        v = tok[rows, :].astype(F32)
        scale = lax.rsqrt(jnp.mean(v * v, axis=-1, keepdims=True) + NORM_EPS)
        normed[rows, :] = (v * scale * gain_ref[...].astype(F32).reshape(1, WIDTH)).astype(BF16)
        return carry

    def project(t, carry):
        cols = pl.ds(pl.multiple_of(t * 256, 256), 256)
        raw[:, cols] = jnp.dot(
            normed[...], full[:, cols], preferred_element_type=F32
        ).astype(BF16)
        return carry

    def glu_rows(t, carry):
        rows = pl.ds(pl.multiple_of(t * 64, 64), 64)
        into = pl.ds(pl.multiple_of(32 + t * 64, 32), 64)
        for c in range(4):
            value = raw[rows, c * 128 : (c + 1) * 128].astype(F32)
            gate = raw[rows, 512 + c * 128 : 640 + c * 128].astype(F32)
            glu = value * jax.nn.sigmoid(gate)
            ext[c, into, :] = glu.astype(BF16).astype(F32)
        return carry

    lane = lax.broadcasted_iota(jnp.int32, (64, 128), 1)
    low_part = lax.rem(lane, 64) < 32

    def table_rows(t, carry):
        rows = pl.ds(pl.multiple_of(t * 64, 64), 64)
        position = me * ROWS + t * 64 + lax.broadcasted_iota(jnp.int32, (64, 128), 0)
        angle = position.astype(F32) * inv_ref[...]
        sine = jnp.sin(angle)
        cos_ref[rows, :] = jnp.cos(angle)
        sin_ref[rows, :] = jnp.where(low_part, -sine, sine)
        return carry

    def rotated(v, rows):
        other = jnp.where(low_part, pltpu.roll(v, 96, 1), pltpu.roll(v, 32, 1))
        return v * cos_ref[rows, :] + other * sin_ref[rows, :]

    def spread(buf, v, into, wide):
        first = jnp.where(wide < 64, v, 0.0)
        second = jnp.where(wide < 64, 0.0, v)
        buf[0, into, :] = first.astype(BF16)
        buf[1, into, :] = pltpu.roll(first, 64, 1).astype(BF16)
        buf[2, into, :] = pltpu.roll(second, 64, 1).astype(BF16)
        buf[3, into, :] = second.astype(BF16)

    def key_rows(t, carry):
        rows = pl.ds(pl.multiple_of(t * 64, 64), 64)
        into = pl.ds(pl.multiple_of(128 + t * 64, 64), 64)
        key = rotated(raw[rows, 1536:1664].astype(F32), rows).astype(BF16)
        spread(kz, key.astype(F32), into, lane)
        spread(vz, raw[rows, 1664:1792].astype(F32), into, lane)
        keep = pl.ds(pl.multiple_of(t * 64, 64), 64)
        halo_send[0, keep, :] = key
        return carry

    def query_rows(t, carry):
        rows = pl.ds(pl.multiple_of(t * 64, 64), 64)
        for c in range(4):
            cols = slice(1024 + c * 128, 1152 + c * 128)
            turned = rotated(raw[rows, cols].astype(F32), rows)
            q_buf[rows, c * 128 : (c + 1) * 128] = (turned * HEAD_DIM**-0.5).astype(BF16)
        return carry

    def conv_rows(t, carry):
        rows = pl.ds(pl.multiple_of(t * 64, 64), 64)
        first = jnp.zeros((64, 128), F32)
        second = jnp.zeros((64, 128), F32)
        for c in range(4):
            near = ext[c, pl.ds(pl.multiple_of(t * 64, 64), 96), :]
            total = None
            for shift in range(8):
                acc = None
                span = 72 if shift else 64
                for whole in range(0, 40, 8):
                    tap = whole + shift - 2
                    if 0 <= tap < 31:
                        term = taps_ref[tap : tap + 1, c * 128 : (c + 1) * 128] * near[whole : whole + span]
                        acc = term if acc is None else acc + term
                acc = acc[shift : shift + 64]
                total = acc if total is None else total + acc
            conv[c, rows, :] = total
            first = first + total
            second = second + total * total
        sums[0, rows, :] = first
        sums[1, rows, :] = second
        return carry

    def branch_rows(t, carry):
        rows = pl.ds(pl.multiple_of(t * 64, 64), 64)
        mean = sums[0, rows, :]
        scale = sums[1, rows, :]
        for c in range(4):
            cols = slice(c * 128, (c + 1) * 128)
            v = (conv[c, rows, :] - mean) * scale * lng_ref[0:1, cols]
            act[rows, cols] = (v * jax.nn.sigmoid(v)).astype(BF16)
        return carry

    seen = lax.broadcasted_iota(jnp.int32, (128, 256), 1)
    asks = lax.broadcasted_iota(jnp.int32, (128, 256), 0)
    head_lane = lax.broadcasted_iota(jnp.int32, (128, 128), 1)

    def attend(t, carry):
        rows = pl.ds(pl.multiple_of(t * 128, 128), 128)
        window = pl.ds(pl.multiple_of(t * 128, 128), 256)
        least = jnp.where(me * SIDE + t == 0, WINDOW, 0)
        allowed = (seen > asks) & (seen <= asks + WINDOW) & (seen >= least)
        logs = jnp.zeros((128, 128), F32)
        for pair in range(4):
            q = q_buf[rows, pair * 128 : (pair + 1) * 128]
            out = None
            for odd in range(2):
                head = 2 * pair + odd
                which = 2 * (pair // 2) + odd
                scores = lax.dot_general(q, kz[which, window, :], NT, preferred_element_type=F32)
                weight = jnp.where(allowed, jnp.exp(scores), 0.0)
                total = jnp.sum(weight, axis=1, keepdims=True)
                total = total + jnp.exp(sinks_ref[0:1, head : head + 1])
                logs = jnp.where(head_lane == head, jnp.log(total), logs)
                weight = (weight * (1.0 / total)).astype(BF16)
                term = jnp.dot(weight, vz[which, window, :], preferred_element_type=F32)
                out = term if out is None else out + term
            act[rows, 512 + pair * 128 : 640 + pair * 128] = out.astype(BF16)
        sums[2, rows, :] = logs
        return carry

    def each(body, g, s, per, start=0):
        def both(t, carry):
            carry = body(t, carry)
            for k in range(per):
                serve(g, s, (t - start) * per + k)
            return carry

        return both

    batch(0, 0, (0,))
    direct(0)
    batch(1, 0, (0,))
    direct(1)
    lax.fori_loop(0, 8, table_rows, 0)
    tok_copy.wait()
    batch(0, 0, range(1, 8))
    lax.fori_loop(0, 5, norm_rows, 0)
    batch(0, 1)
    batch(1, 0, range(1, 8))
    lax.fori_loop(5, 10, norm_rows, 0)
    batch(0, 2)
    batch(1, 1)
    batch(2, 0, (0,))
    direct(2)
    lax.fori_loop(10, 16, norm_rows, 0)
    batch(0, 3)
    batch(1, 2)
    batch(2, 0, range(1, 8))
    batch(0, 4)
    batch(1, 3)
    batch(2, 1)
    from_partner(0)

    lax.fori_loop(0, 2, project, 0)
    lax.fori_loop(2, 4, each(project, 1, 4, 4, 2), 0)
    lax.fori_loop(0, 8, each(glu_rows, 2, 2, 1), 0)
    for c in range(4):
        glu_send[:, c * 128 : (c + 1) * 128] = ext[c, 512:544, :].astype(BF16)
    lax.fori_loop(1, 4, conv_rows, 0)
    go(glu_send, glu_recv, hsend.at[0], hrecv.at[0], after)
    lax.fori_loop(4, 8, conv_rows, 0)
    from_partner(1)
    lax.fori_loop(4, 7, project, 0)
    lax.fori_loop(0, 8, each(key_rows, 2, 3, 1), 0)
    halo_send[1, 384:512, :] = raw[384:512, 1664:1792]
    arrived(glu_recv, hrecv.at[0])
    keep = jnp.where(me == 0, 0.0, 1.0).astype(F32)
    for c in range(4):
        ext[c, 0:32, :] = glu_recv[:, c * 128 : (c + 1) * 128].astype(F32) * keep
    tail = pl.ds(384, 128)
    go(halo_send.at[0, tail], halo_recv.at[0], hsend.at[1], hrecv.at[1], after)
    go(halo_send.at[1, tail], halo_recv.at[1], hsend.at[2], hrecv.at[2], after)
    lax.fori_loop(0, 1, conv_rows, 0)
    stat_send[...] = jnp.zeros((8, ROWS), F32)
    stat_send[0:1, :] = jnp.sum(sums[0].T, axis=0, keepdims=True)
    stat_send[1:2, :] = jnp.sum(sums[1].T, axis=0, keepdims=True)
    for d in (1, 2, 3):
        go(stat_send, stat_recv.at[d - 1], ssend.at[d - 1], srecv.at[d - 1], across(d))
    lax.fori_loop(0, 8, each(query_rows, 2, 4, 1), 0)
    arrived(halo_recv.at[0], hrecv.at[1])
    arrived(halo_recv.at[1], hrecv.at[2])
    for t in range(2):
        rows = slice(t * 64, t * 64 + 64)
        spread(kz, halo_recv[0, rows, :].astype(F32), rows, lane)
        spread(vz, halo_recv[1, rows, :].astype(F32), rows, lane)

    def block(d):
        return lax.rem(x + d + TP, TP)

    def rows_of(d):
        return pl.ds(pl.multiple_of(block(d) * 128, 128), 128)

    def out_part(d, chunks):
        for n in chunks:
            part[n, rows_of(d), :] = lax.dot_general(
                act[rows_of(d), :],
                full[n * 512 : (n + 1) * 512, 1792:2816],
                NT,
                preferred_element_type=F32,
            ).astype(BF16)

    def branch(d):
        lax.fori_loop(2 * block(d), 2 * block(d) + 2, branch_rows, 0)

    inbox = {1: from_low, -1: from_high}

    def send_far(n):
        far = 1 if n < 2 else -1
        go(part.at[n, rows_of(2)], relay_in.at[n], xsend.at[0, n], xrecv.at[0, n], across(far))

    def send_near(n):
        to = -1 if n < 2 else 1
        go(part.at[n, rows_of(to)], inbox[to].at[n], xsend.at[1, n], xrecv.at[1, n], across(to))

    def send_relay(n):
        far = 1 if n < 2 else -1
        arrived(relay_in.at[n], xrecv.at[0, n])
        relay_out[n] = (
            part[n, rows_of(far), :].astype(F32) + relay_in[n].astype(F32)
        ).astype(BF16)
        go(relay_out.at[n], inbox[far].at[n], xsend.at[2, n], xrecv.at[2, n], across(far))

    attend(block(2), 0)
    for d in range(3):
        arrived(stat_recv.at[d], srecv.at[d])
    stats = stat_send[0:2, :] + stat_recv[0, 0:2, :] + stat_recv[1, 0:2, :] + stat_recv[2, 0:2, :]
    stats = stats / CONV_CH
    mean = stats[0:1, :]
    scale = lax.rsqrt(stats[1:2, :] - mean * mean + CHANNEL_EPS)
    sums[0] = jnp.broadcast_to(mean, (128, ROWS)).T
    sums[1] = jnp.broadcast_to(scale, (128, ROWS)).T
    branch(2)
    from_partner(2)
    for n in (0, 2, 1, 3):
        out_part(2, (n,))
        send_far(n)
    attend(block(1), 0)
    branch(1)
    for n in (2, 3):
        out_part(1, (n,))
        send_near(n)
    attend(block(-1), 0)
    branch(-1)
    for n in (0, 1):
        out_part(-1, (n,))
        send_near(n)
    for n in (0, 1):
        out_part(1, (n,))
        send_relay(n)
    for n in (2, 3):
        out_part(-1, (n,))
        send_relay(n)
    attend(block(0), 0)
    branch(0)
    out_part(0, range(4))
    logs_ref[...] = sums[2].T[0:8, :]
    for n in (0, 2, 1, 3):
        arrived(from_low.at[n], xrecv.at[2 if n < 2 else 1, n])
        arrived(from_high.at[n], xrecv.at[1 if n < 2 else 2, n])
        mixed_ref[:, n * 512 : (n + 1) * 512] = (
            part[n, rows_of(0), :].astype(F32)
            + from_low[n].astype(F32)
            + from_high[n].astype(F32)
        ).astype(BF16)
    for copy in started:
        copy.wait_send()
    for g in range(3):
        sent(g)


def hand_on(mixed_in, logs_in, mixed_out, logs_out):
    mixed_out[...] = mixed_in[...]
    logs_out[...] = logs_in[...]


def shards(
    tokens,
    norm_gain,
    w_conv_value,
    w_conv_gate,
    w_query,
    w_key,
    w_value,
    conv_taps,
    ln_gain,
    sinks,
    out_conv,
    out_attn,
):
    half_dim = HEAD_DIM // 2
    inverse = ROPE_BASE ** (-np.arange(half_dim, dtype=np.float32) / half_dim)
    inverse = jnp.asarray(np.tile(inverse.astype(np.float32), 4)[None, :])
    dma = pltpu.SemaphoreType.DMA
    vmem = pl.BlockSpec(memory_space=pltpu.VMEM)
    V = pltpu.VMEM
    mixed, logs = pl.pallas_call(
        kernel,
        out_shape=(
            jax.ShapeDtypeStruct((128, WIDTH), BF16),
            jax.ShapeDtypeStruct((8, ROWS), F32),
        ),
        in_specs=[pl.BlockSpec(memory_space=pl.ANY)] + [vmem] * 12,
        out_specs=(vmem, vmem),
        scratch_shapes=[
            V((WIDTH, 2816), BF16),
            V((16, 2816), BF16),
            V((ROWS, WIDTH), BF16),
            V((ROWS, WIDTH), BF16),
            V((ROWS, 1792), BF16),
            V((4, 544, 128), F32),
            V((4, ROWS, 128), F32),
            V((3, ROWS, 128), F32),
            V((ROWS, 512), BF16),
            V((4, 640, 128), BF16),
            V((4, 640, 128), BF16),
            V((ROWS, 1024), BF16),
            V((2, ROWS, 128), BF16),
            V((2, 128, 128), BF16),
            V((32, 512), BF16),
            V((32, 512), BF16),
            V((8, ROWS), F32),
            V((3, 8, ROWS), F32),
            V((4, ROWS, 512), BF16),
            V((4, 128, 512), BF16),
            V((4, 128, 512), BF16),
            V((4, 128, 512), BF16),
            V((4, 128, 512), BF16),
            dma,
            dma((3, 8)),
            dma((3, 8, 9)),
            dma((3,)),
            dma((3,)),
            dma((3,)),
            dma((3,)),
            dma((3,)),
            dma((3,)),
            dma((3, 4)),
            dma((3, 4)),
            V((ROWS, 128), F32),
            V((ROWS, 128), F32),
        ],
        compiler_params=pltpu.CompilerParams(collective_id=0, has_side_effects=True),
        name="layer",
    )(
        tokens,
        norm_gain,
        w_conv_value,
        w_conv_gate,
        w_query,
        w_key,
        w_value,
        conv_taps,
        ln_gain.reshape(1, 512),
        sinks.reshape(1, 8),
        out_conv.T,
        out_attn.T,
        inverse,
    )
    return pl.pallas_call(
        hand_on,
        out_shape=(
            jax.ShapeDtypeStruct((128, WIDTH), BF16),
            jax.ShapeDtypeStruct((8, ROWS), F32),
        ),
        in_specs=[vmem, vmem],
        out_specs=(vmem, vmem),
        name="hand_on",
    )(mixed, logs)


def solution(mesh):
    in_specs = (
        P("sp", None),
        P(),
        P("sp", "tp"),
        P("sp", "tp"),
        P("sp", "tp"),
        P("sp", "tp"),
        P("sp", "tp"),
        P(None, "tp"),
        P("tp"),
        P("tp"),
        P("tp", "sp"),
        P("tp", "sp"),
    )
    out_specs = (P(("sp", "tp"), None), P("tp", "sp"))
    return jax.shard_map(shards, mesh=mesh, in_specs=in_specs, out_specs=out_specs, check_vma=False)
```

```python
import jax
import jax.numpy as jnp
import numpy as np
from jax import lax
from jax.experimental import pallas as pl
from jax.experimental.pallas import tpu as pltpu
from jax.sharding import PartitionSpec as P

CONV_CH = 2048
HEADS = 32
KV_HEADS = 8
HEAD_DIM = 64
WINDOW = 128
NORM_EPS = 1e-06
CHANNEL_EPS = 1e-05
ROPE_BASE = 10000.0
MESH = pl.DeviceIdType.MESH
F32 = jnp.float32
BF16 = jnp.bfloat16

SIDE = 8
TP = 4
ROWS = 512
WIDTH = 2048
GROUPS = ((0, 1024), (1024, 1792), (1792, 2816))
ORDER = (0, 1, -1, 2, -2, 3, -3, 4)
NT = (((1,), (1,)), ((), ()))


def kernel(
    tokens_ref,
    gain_ref,
    wcv_ref,
    wcg_ref,
    wq_ref,
    wk_ref,
    wv_ref,
    taps_ref,
    lng_ref,
    sinks_ref,
    oc_ref,
    oa_ref,
    inv_ref,
    mixed_ref,
    logs_ref,
    full,
    piece,
    tok,
    normed,
    raw,
    ext,
    conv,
    sums,
    q_buf,
    kz,
    vz,
    act,
    halo_send,
    halo_recv,
    glu_send,
    glu_recv,
    stat_send,
    stat_recv,
    part,
    relay_in,
    relay_out,
    from_low,
    from_high,
    tok_sem,
    drecv,
    rrecv,
    precv,
    gsend,
    hsend,
    hrecv,
    ssend,
    srecv,
    xsend,
    xrecv,
    cos_ref,
    sin_ref,
):
    me = lax.axis_index("sp")
    x = lax.axis_index("tp")
    core = lax.rem(me, 2)
    y = lax.rem(me // 2, SIDE)
    z = me // (2 * SIDE)

    def device(zz, yy, cc):
        return {"sp": (zz * SIDE + yy) * 2 + cc}

    def wrap(v):
        return lax.rem(v + 2 * SIDE, SIDE)

    def at(a, b, c):
        return wrap(z + (1 - c) * a + c * b), wrap(y + (1 - c) * b + c * a)

    def peer(a, b):
        return device(*at(a, b, core), core)

    def across(d):
        return {"tp": lax.rem(x + d + TP, TP)}

    partner = device(z, y, 1 - core)
    count = 2 * SIDE * SIDE
    after = {"sp": lax.rem(me + 1, count)}
    before = {"sp": lax.rem(me + count - 1, count)}
    started = []

    def remote(src, dst, send, recv, to):
        return pltpu.make_async_remote_copy(
            src_ref=src,
            dst_ref=dst,
            send_sem=send,
            recv_sem=recv,
            device_id=to,
            device_id_type=MESH,
        )

    def go(src, dst, send, recv, to):
        copy = remote(src, dst, send, recv, to)
        copy.start()
        started.append(copy)

    tok_copy = pltpu.make_async_copy(tokens_ref, tok, tok_sem)
    tok_copy.start()
    piece[:, 0:512] = wcv_ref[...]
    piece[:, 512:1024] = wcg_ref[...]
    piece[:, 1024:1536] = wq_ref[...]
    piece[:, 1536:1664] = wk_ref[...]
    piece[:, 1664:1792] = wv_ref[...]
    piece[:, 1792:2304] = oc_ref[...]
    piece[:, 2304:2816] = oa_ref[...]
    full[pl.ds(pl.multiple_of(me * 16, 16), 16), :] = piece[...]

    greeted = [peer(a, 0) for a in ORDER[1:]] + [peer(0, 1), peer(0, -1), partner]
    greeted += [after, before] + [across(d) for d in (1, 2, 3)]
    barrier = pltpu.get_barrier_semaphore()
    for one in greeted:
        pl.semaphore_signal(barrier, inc=1, device_id=one, device_id_type=MESH)
    pl.semaphore_wait(barrier, len(greeted))

    def slot(g, a, b, c=None, half=None):
        c = core if c is None else c
        zz, yy = at(-a, -b, c)
        low, high = GROUPS[g]
        width = high - low
        if half is not None:
            width = width // 2
            low = low + half * width
        row = pl.multiple_of(((zz * SIDE + yy) * 2 + c) * 16, 16)
        return full.at[pl.ds(row, 16), pl.ds(low, width)]

    def own(g):
        low, high = GROUPS[g]
        return piece.at[:, pl.ds(low, high - low)]

    def direct(g):
        for i, a in enumerate(ORDER):
            if a:
                remote(own(g), slot(g, 0, 0), gsend.at[g], drecv.at[g, i], peer(a, 0)).start()

    def arrived(ref, sem):
        remote(ref, ref, hsend.at[0], sem, partner).wait_recv()

    def place(i):
        if isinstance(i, int):
            return ORDER[i]
        return (i + 1) // 2 * (2 * lax.rem(i, 2) - 1)

    def serve(g, s, i):
        a = place(i)

        def ring(src, ref, b, recv):
            remote(src, ref, gsend.at[g], recv, peer(0, 1 if b > 0 else -1)).start()

        def share(src, ref):
            remote(src, ref, gsend.at[g], precv.at[g], partner).start()

        if s == 0:
            ref = slot(g, a, 0)
            if a:
                arrived(ref, drecv.at[g, i])
            src = ref if a else own(g)
            for b in (1, -1):
                ring(src, ref, b, rrecv.at[g, i, 3 + b])
            share(src, ref)
        elif s < 4:
            for sign in (1, -1):
                ref = slot(g, a, sign * s)
                arrived(ref, rrecv.at[g, i, 3 + sign * s])
                if s < 3:
                    b = sign * (s + 1)
                    ring(ref, ref, b, rrecv.at[g, i, 3 + b])
                else:
                    h = 0 if sign > 0 else 1
                    out = slot(g, a, sign * s, half=h)
                    ring(out, out, sign, rrecv.at[g, i, 7 + h])
                share(ref, ref)
        else:
            for h in range(2):
                arrived(slot(g, a, 4, half=h), rrecv.at[g, i, 7 + h])
            share(slot(g, a, 4), slot(g, a, 4))

    def batch(g, s, items=range(8)):
        for i in items:
            serve(g, s, i)

    def rows_in(g, count):
        low, high = GROUPS[g]
        return full.at[pl.ds(0, count), pl.ds(low, high - low)]

    def from_partner(g):
        arrived(rows_in(g, 1024), precv.at[g])

    def sent(g):
        ref = rows_in(g, 127 * 16)
        remote(ref, ref, gsend.at[g], tok_sem, partner).wait_send()

    def norm_rows(t, carry):
        rows = pl.ds(pl.multiple_of(t * 32, 32), 32)
        v = tok[rows, :].astype(F32)
        scale = lax.rsqrt(jnp.mean(v * v, axis=-1, keepdims=True) + NORM_EPS)
        normed[rows, :] = (v * scale * gain_ref[...].astype(F32).reshape(1, WIDTH)).astype(BF16)
        return carry

    def project(t, carry):
        cols = pl.ds(pl.multiple_of(t * 256, 256), 256)
        raw[:, cols] = jnp.dot(
            normed[...], full[:, cols], preferred_element_type=F32
        ).astype(BF16)
        return carry

    def glu_rows(t, carry):
        rows = pl.ds(pl.multiple_of(t * 64, 64), 64)
        into = pl.ds(pl.multiple_of(32 + t * 64, 32), 64)
        for c in range(4):
            value = raw[rows, c * 128 : (c + 1) * 128].astype(F32)
            gate = raw[rows, 512 + c * 128 : 640 + c * 128].astype(F32)
            glu = value * jax.nn.sigmoid(gate)
            ext[c, into, :] = glu.astype(BF16).astype(F32)
        return carry

    lane = lax.broadcasted_iota(jnp.int32, (64, 128), 1)
    low_part = lax.rem(lane, 64) < 32

    def table_rows(t, carry):
        rows = pl.ds(pl.multiple_of(t * 64, 64), 64)
        position = me * ROWS + t * 64 + lax.broadcasted_iota(jnp.int32, (64, 128), 0)
        angle = position.astype(F32) * inv_ref[...]
        sine = jnp.sin(angle)
        cos_ref[rows, :] = jnp.cos(angle)
        sin_ref[rows, :] = jnp.where(low_part, -sine, sine)
        return carry

    def rotated(v, rows):
        other = jnp.where(low_part, pltpu.roll(v, 96, 1), pltpu.roll(v, 32, 1))
        return v * cos_ref[rows, :] + other * sin_ref[rows, :]

    def spread(buf, v, into, wide):
        first = jnp.where(wide < 64, v, 0.0)
        second = jnp.where(wide < 64, 0.0, v)
        buf[0, into, :] = first.astype(BF16)
        buf[1, into, :] = pltpu.roll(first, 64, 1).astype(BF16)
        buf[2, into, :] = pltpu.roll(second, 64, 1).astype(BF16)
        buf[3, into, :] = second.astype(BF16)

    def key_rows(t, carry):
        rows = pl.ds(pl.multiple_of(t * 64, 64), 64)
        into = pl.ds(pl.multiple_of(128 + t * 64, 64), 64)
        key = rotated(raw[rows, 1536:1664].astype(F32), rows).astype(BF16)
        spread(kz, key.astype(F32), into, lane)
        spread(vz, raw[rows, 1664:1792].astype(F32), into, lane)
        keep = pl.ds(pl.multiple_of(t * 64, 64), 64)
        halo_send[0, keep, :] = key
        return carry

    def query_rows(t, carry):
        rows = pl.ds(pl.multiple_of(t * 64, 64), 64)
        for c in range(4):
            cols = slice(1024 + c * 128, 1152 + c * 128)
            turned = rotated(raw[rows, cols].astype(F32), rows)
            q_buf[rows, c * 128 : (c + 1) * 128] = (turned * HEAD_DIM**-0.5).astype(BF16)
        return carry

    def conv_rows(t, carry):
        rows = pl.ds(pl.multiple_of(t * 64, 64), 64)
        first = jnp.zeros((64, 128), F32)
        second = jnp.zeros((64, 128), F32)
        for c in range(4):
            near = ext[c, pl.ds(pl.multiple_of(t * 64, 64), 96), :]
            total = None
            for shift in range(8):
                acc = None
                span = 72 if shift else 64
                for whole in range(0, 40, 8):
                    tap = whole + shift - 2
                    if 0 <= tap < 31:
                        term = taps_ref[tap : tap + 1, c * 128 : (c + 1) * 128] * near[whole : whole + span]
                        acc = term if acc is None else acc + term
                acc = acc[shift : shift + 64]
                total = acc if total is None else total + acc
            conv[c, rows, :] = total
            first = first + total
            second = second + total * total
        sums[0, rows, :] = first
        sums[1, rows, :] = second
        return carry

    def branch_rows(t, carry):
        rows = pl.ds(pl.multiple_of(t * 64, 64), 64)
        mean = sums[0, rows, :]
        scale = sums[1, rows, :]
        for c in range(4):
            cols = slice(c * 128, (c + 1) * 128)
            v = (conv[c, rows, :] - mean) * scale * lng_ref[0:1, cols]
            act[rows, cols] = (v * jax.nn.sigmoid(v)).astype(BF16)
        return carry

    seen = lax.broadcasted_iota(jnp.int32, (128, 256), 1)
    asks = lax.broadcasted_iota(jnp.int32, (128, 256), 0)
    head_lane = lax.broadcasted_iota(jnp.int32, (128, 128), 1)

    def attend(t, carry):
        rows = pl.ds(pl.multiple_of(t * 128, 128), 128)
        window = pl.ds(pl.multiple_of(t * 128, 128), 256)
        least = jnp.where(me * SIDE + t == 0, WINDOW, 0)
        allowed = (seen > asks) & (seen <= asks + WINDOW) & (seen >= least)
        logs = jnp.zeros((128, 128), F32)
        for pair in range(4):
            q = q_buf[rows, pair * 128 : (pair + 1) * 128]
            out = None
            for odd in range(2):
                head = 2 * pair + odd
                which = 2 * (pair // 2) + odd
                scores = lax.dot_general(q, kz[which, window, :], NT, preferred_element_type=F32)
                weight = jnp.where(allowed, jnp.exp(scores), 0.0)
                total = jnp.sum(weight, axis=1, keepdims=True)
                total = total + jnp.exp(sinks_ref[0:1, head : head + 1])
                logs = jnp.where(head_lane == head, jnp.log(total), logs)
                weight = (weight * (1.0 / total)).astype(BF16)
                term = jnp.dot(weight, vz[which, window, :], preferred_element_type=F32)
                out = term if out is None else out + term
            act[rows, 512 + pair * 128 : 640 + pair * 128] = out.astype(BF16)
        sums[2, rows, :] = logs
        return carry

    def each(body, g, s, per, start=0):
        def both(t, carry):
            carry = body(t, carry)
            for k in range(per):
                serve(g, s, (t - start) * per + k)
            return carry

        return both

    batch(0, 0, (0,))
    direct(0)
    batch(1, 0, (0,))
    direct(1)
    lax.fori_loop(0, 8, table_rows, 0)
    tok_copy.wait()
    batch(0, 0, range(1, 8))
    lax.fori_loop(0, 5, norm_rows, 0)
    batch(0, 1)
    batch(1, 0, range(1, 8))
    lax.fori_loop(5, 10, norm_rows, 0)
    batch(0, 2)
    batch(1, 1)
    batch(2, 0, (0,))
    direct(2)
    lax.fori_loop(10, 16, norm_rows, 0)
    batch(0, 3)
    batch(1, 2)
    batch(2, 0, range(1, 8))
    batch(0, 4)
    from_partner(0)

    lax.fori_loop(0, 2, project, 0)
    batch(1, 3)
    batch(2, 1)
    lax.fori_loop(2, 4, project, 0)
    lax.fori_loop(0, 8, glu_rows, 0)
    for c in range(4):
        glu_send[:, c * 128 : (c + 1) * 128] = ext[c, 512:544, :].astype(BF16)
    lax.fori_loop(1, 4, conv_rows, 0)
    go(glu_send, glu_recv, hsend.at[0], hrecv.at[0], after)
    lax.fori_loop(4, 8, each(each(conv_rows, 1, 4, 2, 4), 2, 2, 2, 4), 0)
    from_partner(1)
    lax.fori_loop(4, 7, project, 0)
    batch(2, 3)
    lax.fori_loop(0, 8, key_rows, 0)
    halo_send[1, 384:512, :] = raw[384:512, 1664:1792]
    arrived(glu_recv, hrecv.at[0])
    keep = jnp.where(me == 0, 0.0, 1.0).astype(F32)
    for c in range(4):
        ext[c, 0:32, :] = glu_recv[:, c * 128 : (c + 1) * 128].astype(F32) * keep
    tail = pl.ds(384, 128)
    go(halo_send.at[0, tail], halo_recv.at[0], hsend.at[1], hrecv.at[1], after)
    go(halo_send.at[1, tail], halo_recv.at[1], hsend.at[2], hrecv.at[2], after)
    lax.fori_loop(0, 1, conv_rows, 0)
    stat_send[...] = jnp.zeros((8, ROWS), F32)
    stat_send[0:1, :] = jnp.sum(sums[0].T, axis=0, keepdims=True)
    stat_send[1:2, :] = jnp.sum(sums[1].T, axis=0, keepdims=True)
    for d in (1, 2, 3):
        go(stat_send, stat_recv.at[d - 1], ssend.at[d - 1], srecv.at[d - 1], across(d))
    lax.fori_loop(0, 8, each(query_rows, 2, 4, 1), 0)
    arrived(halo_recv.at[0], hrecv.at[1])
    arrived(halo_recv.at[1], hrecv.at[2])
    for t in range(2):
        rows = slice(t * 64, t * 64 + 64)
        spread(kz, halo_recv[0, rows, :].astype(F32), rows, lane)
        spread(vz, halo_recv[1, rows, :].astype(F32), rows, lane)

    def block(d):
        return lax.rem(x + d + TP, TP)

    def rows_of(d):
        return pl.ds(pl.multiple_of(block(d) * 128, 128), 128)

    def out_part(d, chunks):
        for n in chunks:
            part[n, rows_of(d), :] = lax.dot_general(
                act[rows_of(d), :],
                full[n * 512 : (n + 1) * 512, 1792:2816],
                NT,
                preferred_element_type=F32,
            ).astype(BF16)

    def branch(d):
        lax.fori_loop(2 * block(d), 2 * block(d) + 2, branch_rows, 0)

    inbox = {1: from_low, -1: from_high}

    def send_far(n):
        far = 1 if n < 2 else -1
        go(part.at[n, rows_of(2)], relay_in.at[n], xsend.at[0, n], xrecv.at[0, n], across(far))

    def send_near(n):
        to = -1 if n < 2 else 1
        go(part.at[n, rows_of(to)], inbox[to].at[n], xsend.at[1, n], xrecv.at[1, n], across(to))

    def send_relay(n):
        far = 1 if n < 2 else -1
        arrived(relay_in.at[n], xrecv.at[0, n])
        relay_out[n] = (
            part[n, rows_of(far), :].astype(F32) + relay_in[n].astype(F32)
        ).astype(BF16)
        go(relay_out.at[n], inbox[far].at[n], xsend.at[2, n], xrecv.at[2, n], across(far))

    attend(block(2), 0)
    for d in range(3):
        arrived(stat_recv.at[d], srecv.at[d])
    stats = stat_send[0:2, :] + stat_recv[0, 0:2, :] + stat_recv[1, 0:2, :] + stat_recv[2, 0:2, :]
    stats = stats / CONV_CH
    mean = stats[0:1, :]
    scale = lax.rsqrt(stats[1:2, :] - mean * mean + CHANNEL_EPS)
    sums[0] = jnp.broadcast_to(mean, (128, ROWS)).T
    sums[1] = jnp.broadcast_to(scale, (128, ROWS)).T
    branch(2)
    from_partner(2)
    for n in (0, 2, 1, 3):
        out_part(2, (n,))
        send_far(n)
    attend(block(1), 0)
    branch(1)
    for n in (2, 3):
        out_part(1, (n,))
        send_near(n)
    attend(block(-1), 0)
    branch(-1)
    for n in (0, 1):
        out_part(-1, (n,))
        send_near(n)
    for n in (0, 1):
        out_part(1, (n,))
        send_relay(n)
    for n in (2, 3):
        out_part(-1, (n,))
        send_relay(n)
    attend(block(0), 0)
    branch(0)
    out_part(0, range(4))
    logs_ref[...] = sums[2].T[0:8, :]
    for n in (0, 2, 1, 3):
        arrived(from_low.at[n], xrecv.at[2 if n < 2 else 1, n])
        arrived(from_high.at[n], xrecv.at[1 if n < 2 else 2, n])
        mixed_ref[:, n * 512 : (n + 1) * 512] = (
            part[n, rows_of(0), :].astype(F32)
            + from_low[n].astype(F32)
            + from_high[n].astype(F32)
        ).astype(BF16)
    for copy in started:
        copy.wait_send()
    for g in range(3):
        sent(g)


def hand_on(mixed_in, logs_in, mixed_out, logs_out):
    mixed_out[...] = mixed_in[...]
    logs_out[...] = logs_in[...]


def shards(
    tokens,
    norm_gain,
    w_conv_value,
    w_conv_gate,
    w_query,
    w_key,
    w_value,
    conv_taps,
    ln_gain,
    sinks,
    out_conv,
    out_attn,
):
    half_dim = HEAD_DIM // 2
    inverse = ROPE_BASE ** (-np.arange(half_dim, dtype=np.float32) / half_dim)
    inverse = jnp.asarray(np.tile(inverse.astype(np.float32), 4)[None, :])
    dma = pltpu.SemaphoreType.DMA
    vmem = pl.BlockSpec(memory_space=pltpu.VMEM)
    V = pltpu.VMEM
    mixed, logs = pl.pallas_call(
        kernel,
        out_shape=(
            jax.ShapeDtypeStruct((128, WIDTH), BF16),
            jax.ShapeDtypeStruct((8, ROWS), F32),
        ),
        in_specs=[pl.BlockSpec(memory_space=pl.ANY)] + [vmem] * 12,
        out_specs=(vmem, vmem),
        scratch_shapes=[
            V((WIDTH, 2816), BF16),
            V((16, 2816), BF16),
            V((ROWS, WIDTH), BF16),
            V((ROWS, WIDTH), BF16),
            V((ROWS, 1792), BF16),
            V((4, 544, 128), F32),
            V((4, ROWS, 128), F32),
            V((3, ROWS, 128), F32),
            V((ROWS, 512), BF16),
            V((4, 640, 128), BF16),
            V((4, 640, 128), BF16),
            V((ROWS, 1024), BF16),
            V((2, ROWS, 128), BF16),
            V((2, 128, 128), BF16),
            V((32, 512), BF16),
            V((32, 512), BF16),
            V((8, ROWS), F32),
            V((3, 8, ROWS), F32),
            V((4, ROWS, 512), BF16),
            V((4, 128, 512), BF16),
            V((4, 128, 512), BF16),
            V((4, 128, 512), BF16),
            V((4, 128, 512), BF16),
            dma,
            dma((3, 8)),
            dma((3, 8, 9)),
            dma((3,)),
            dma((3,)),
            dma((3,)),
            dma((3,)),
            dma((3,)),
            dma((3,)),
            dma((3, 4)),
            dma((3, 4)),
            V((ROWS, 128), F32),
            V((ROWS, 128), F32),
        ],
        compiler_params=pltpu.CompilerParams(collective_id=0, has_side_effects=True),
        name="layer",
    )(
        tokens,
        norm_gain,
        w_conv_value,
        w_conv_gate,
        w_query,
        w_key,
        w_value,
        conv_taps,
        ln_gain.reshape(1, 512),
        sinks.reshape(1, 8),
        out_conv.T,
        out_attn.T,
        inverse,
    )
    return pl.pallas_call(
        hand_on,
        out_shape=(
            jax.ShapeDtypeStruct((128, WIDTH), BF16),
            jax.ShapeDtypeStruct((8, ROWS), F32),
        ),
        in_specs=[vmem, vmem],
        out_specs=(vmem, vmem),
        name="hand_on",
    )(mixed, logs)


def solution(mesh):
    in_specs = (
        P("sp", None),
        P(),
        P("sp", "tp"),
        P("sp", "tp"),
        P("sp", "tp"),
        P("sp", "tp"),
        P("sp", "tp"),
        P(None, "tp"),
        P("tp"),
        P("tp"),
        P("tp", "sp"),
        P("tp", "sp"),
    )
    out_specs = (P(("sp", "tp"), None), P("tp", "sp"))
    return jax.shard_map(shards, mesh=mesh, in_specs=in_specs, out_specs=out_specs, check_vma=False)
```
